32 devices in a mesh: ep: 16 (over z, x, core), tp: 2 (over y).
Axes of the slice: x: 2, y: 2, z: 4, core: 2. Of those that a mesh axis runs over, the one named last changes fastest.
Arguments:
- tokens: bfloat16 [256, 1024], P('ep'), may hold values from -6 to 6
- state: float32 [256, 16, 64, 64], P('ep', 'tp'), may hold values from -6 to 6
- w_recep: bfloat16 [1024, 1024], P(None, 'tp'), may hold values from -0.1875 to 0.1875
- w_key: bfloat16 [1024, 1024], P(None, 'tp'), may hold values from -0.1875 to 0.1875
- w_value: bfloat16 [1024, 1024], P(None, 'tp'), may hold values from -0.1875 to 0.1875
- w_out: bfloat16 [1024, 1024], P('tp'), may hold values from -0.1875 to 0.1875
- decay_base: float32 [1024], P('tp'), may hold values from -5 to 1
- decay_down: bfloat16 [1024, 64], replicated, may hold values from -0.1875 to 0.1875
- decay_up: bfloat16 [64, 1024], P(None, 'tp'), may hold values from -1 to 1
- rate_base: float32 [1024], P('tp'), may hold values from -4 to 4
- rate_down: bfloat16 [1024, 64], replicated, may hold values from -0.1875 to 0.1875
- rate_up: bfloat16 [64, 1024], P(None, 'tp'), may hold values from -1 to 1
- head_gain: float32 [1024], P('tp'), may hold values from 0.1 to 1.9
- first_gain: float32 [1024], replicated, may hold values from 0.2 to 4.8
- expert_gate: bfloat16 [16, 1024, 1408], P('ep', None, 'tp'), may hold values from -0.1875 to 0.1875
- expert_up: bfloat16 [16, 1024, 1408], P('ep', None, 'tp'), may hold values from -0.1875 to 0.1875
- expert_down: bfloat16 [16, 1408, 1024], P('ep', 'tp'), may hold values from -0.078125 to 0.078125
- dense_gate: bfloat16 [2816, 1024], P('ep'), may hold values from -0.1875 to 0.1875
- dense_up: bfloat16 [2816, 1024], P('ep'), may hold values from -0.1875 to 0.1875
- dense_down: bfloat16 [2816, 1024], P('ep', 'tp'), may hold values from -0.21875 to 0.21875
- branch_gate: bfloat16 [1024], replicated, may hold values from -0.1875 to 0.1875
- second_gain: float32 [1024], P('tp'), may hold values from 0.1 to 1.9
- routes: int32 [256, 2], P('ep'), may hold values from 0 to 3, all different within a row; in each aligned block of 16 rows (0 to 15, 16 to 31, ...) at most 16 rows name the same one
- route_weights: float32 [256, 2], P('ep'), may hold values from 0.2 to 1
Outputs:
- layer_output: bfloat16 [256, 1024], P('ep', 'tp')
The draws below stay inside these ranges and needn't reach their ends.
Inputs may be any that keep to these rules, and one draw needn't show every extreme that they name: `routes`: each row names 2 different experts. In each aligned block of 16 rows no expert is named by more than 16 rows, a bound that some block reaches.
All inputs are finite; a program needn't handle non-finite values.
Results may differ from the reference program's by a relative error of at most 0.018.
Values may be sent and summed in bfloat16 or wider, within the bound.
A program may use at most 64 MiB of HBM per device.

```python
import math
from functools import partial
import jax
import jax.numpy as jnp
import numpy as np
from jax import lax

MODEL_DIMENSION = 1024
HEAD = 64
RANK = 64
FF_E = 5632
FF_D = 2816
SPLIT = 4
TOP_K = 2
B_DEV = 16
HEADS = 16
TOKEN_TOTAL = 256
EXPERTS = 4
CAP = 16
N_EP = 16


def draw_first_gain(key, part):
    position = jnp.arange(MODEL_DIMENSION, dtype=jnp.float32) / MODEL_DIMENSION
    jitter = jax.random.uniform(key, (MODEL_DIMENSION,), jnp.float32, 0.0, 1.0)
    return (0.5 + jitter) * jnp.exp(jnp.log(3.0) * position) * 0.6


def block_levels(rng, dims, shards, low, top_value):
    def one(dim, shards_of):
        draws = jax.random.uniform(jax.random.fold_in(jax.random.fold_in(rng, 6), dim), (shards_of,), jnp.float32, low / len(shards), top_value / len(shards))
        return jnp.repeat(jnp.exp(draws), dims[dim] // shards_of).reshape((-1,) + (1,) * (len(dims) - dim - 1))

    loudness = one(*shards[0])
    for cut in shards[1:]:
        loudness = loudness * one(*cut)
    return loudness


def shared_out(stream_key, own, number, rows, count, top, limit, skew):
    sequence = jax.random.permutation(stream_key, count)
    crowded, ordinary = load_shares(count, rows * top, limit, skew, True), load_shares(count, rows * top, limit, skew, False)
    places = jnp.arange(count)

    def named(lengths, turn):
        used = int((lengths > 0).sum())
        fixed = max(1, used // 4)
        passed = fixed + (places - fixed + turn * (used - fixed)) % max(1, count - fixed)
        return jnp.zeros((count,), jnp.int32).at[sequence[jnp.where(places < fixed, places, passed)]].set(jnp.asarray(lengths, jnp.int32))

    lengths = jnp.where(number % 4 == 0, named(crowded, number // 4), named(ordinary, number - number // 4 - 1))
    mixed = jax.random.permutation(jax.random.fold_in(own, 3), count)
    donor, taker = mixed[0:count // 2 * 2:2], mixed[1:count // 2 * 2:2]
    room = jnp.minimum(lengths[donor] - 1, limit - lengths[taker]) // 2
    room = jnp.where((donor == sequence[0]) | (taker == sequence[0]) | (lengths[taker] == 0), 0, jnp.maximum(room, 0))
    passed = jax.random.randint(jax.random.fold_in(own, 4), (count // 2,), 0, 1 << 20) % (room + 1)
    lengths = lengths.at[donor].add(-passed).at[taker].add(passed)
    items = jnp.searchsorted(jnp.cumsum(lengths), jnp.arange(rows * top), side="right").astype(jnp.int32)
    grid = items.reshape(top, rows).T
    grid = grid[jax.random.permutation(jax.random.fold_in(own, 1), rows)]
    turn = jax.random.randint(jax.random.fold_in(own, 2), (rows, 1), 0, top)
    return jnp.take_along_axis(grid, (jnp.arange(top)[None, :] + turn) % top, axis=1)


def load_shares(count, total, bound, slope, full):
    loads = [(1 << 20) // math.isqrt(rank ** slope) + 1 for rank in range(1, count + 1)]
    largest = bound if full else min(bound, max(-(-total // count), total * loads[0] // sum(loads)))
    least = 1 if total - largest >= count - 1 else 0
    holding, rest = [largest] + [least] * (count - 1), total - largest - least * (count - 1)
    while rest > 0:
        movable = [i for i in range(1, count) if holding[i] < largest] or [i for i in range(1, count) if holding[i] < bound]
        mass, left = sum([loads[i] for i in movable]), rest
        for i in movable:
            more = min(bound - holding[i], max(1, left * loads[i] // mass), rest)
            holding[i] = holding[i] + more
            rest = rest - more
    return np.array(holding)


def noise(key, shape, scale, reach, shards=(), held_as=jnp.bfloat16):
    values = jax.random.normal(key, shape, jnp.float32) * scale
    if len(shards) > 0:
        values = block_levels(key, shape, shards, -0.22, 0.18) * values
    return jnp.clip(values, min=-reach, max=reach).astype(held_as)


def setup_inputs(seed: int = 0) -> dict:
    key_list = jax.random.split(jax.random.key(seed), 25)
    tokens = noise(key_list[0], (TOKEN_TOTAL, MODEL_DIMENSION), 1.0, 6.0, ((0, 16),))
    state = noise(key_list[1], (TOKEN_TOTAL, HEADS, HEAD, HEAD), 1.0, 6.0, ((0, 16), (1, 2)), jnp.float32)
    w_recep = noise(key_list[2], (MODEL_DIMENSION, MODEL_DIMENSION), MODEL_DIMENSION ** -0.5, 0.1875, ((1, 2),))
    w_key = noise(key_list[3], (MODEL_DIMENSION, MODEL_DIMENSION), MODEL_DIMENSION ** -0.5, 0.1875, ((1, 2),))
    w_value = noise(key_list[4], (MODEL_DIMENSION, MODEL_DIMENSION), MODEL_DIMENSION ** -0.5, 0.1875, ((1, 2),))
    w_out = noise(key_list[5], (MODEL_DIMENSION, MODEL_DIMENSION), MODEL_DIMENSION ** -0.5, 0.1875, ((0, 2),))
    decay_base = jnp.clip(-5.0 + 6.0 * jax.random.uniform(key_list[6], (MODEL_DIMENSION,), jnp.float32) ** block_levels(key_list[6], (MODEL_DIMENSION,), ((0, 2),), -0.2, 0.2), -5.0, 1.0)
    decay_down = noise(key_list[7], (MODEL_DIMENSION, RANK), MODEL_DIMENSION ** -0.5, 0.1875)
    decay_up = noise(key_list[8], (RANK, MODEL_DIMENSION), (RANK // 2) ** -0.5, 1.0, ((1, 2),))
    rate_base = noise(key_list[9], (MODEL_DIMENSION,), 1.0, 4.0, ((0, 2),), jnp.float32)
    rate_down = noise(key_list[10], (MODEL_DIMENSION, RANK), MODEL_DIMENSION ** -0.5, 0.1875)
    rate_up = noise(key_list[11], (RANK, MODEL_DIMENSION), (RANK // 2) ** -0.5, 1.0, ((1, 2),))
    head_gain = jnp.clip(1.0 + 0.18 * jax.random.normal(key_list[12], (MODEL_DIMENSION,), jnp.float32), 0.1, 1.9)
    first_gain = draw_first_gain(jax.random.fold_in(key_list[24], 71), 0)
    expert_gate = noise(key_list[14], (N_EP, MODEL_DIMENSION, FF_E // SPLIT), MODEL_DIMENSION ** -0.5, 0.1875, ((0, 16), (2, 2)))
    expert_up = noise(key_list[15], (N_EP, MODEL_DIMENSION, FF_E // SPLIT), MODEL_DIMENSION ** -0.5, 0.1875, ((0, 16), (2, 2)))
    expert_down = noise(key_list[16], (N_EP, FF_E // SPLIT, MODEL_DIMENSION), FF_E ** -0.5, 0.078125, ((0, 16), (1, 2)))
    dense_gate = noise(key_list[17], (FF_D, MODEL_DIMENSION), MODEL_DIMENSION ** -0.5, 0.1875, ((0, 16),))
    dense_up = noise(key_list[18], (FF_D, MODEL_DIMENSION), MODEL_DIMENSION ** -0.5, 0.1875, ((0, 16),))
    dense_down = noise(key_list[19], (FF_D, MODEL_DIMENSION), (FF_D // 4) ** -0.5, 0.21875, ((0, 16), (1, 2)))
    branch_gate = noise(key_list[20], (MODEL_DIMENSION,), MODEL_DIMENSION ** -0.5, 0.1875)
    second_gain = jnp.clip(1.0 + 0.18 * jax.random.normal(key_list[21], (MODEL_DIMENSION,), jnp.float32), 0.1, 1.9)
    routes_keys = jax.random.split(jax.random.fold_in(key_list[22], 1), TOKEN_TOTAL // B_DEV)
    routes_turns = jax.random.permutation(jax.random.fold_in(key_list[22], 3), TOKEN_TOTAL // B_DEV)
    routes = jax.vmap(lambda own, number: shared_out(jax.random.fold_in(key_list[22], 2), own, number, B_DEV, EXPERTS, TOP_K, CAP, 2))(routes_keys, routes_turns).reshape((TOKEN_TOTAL, TOP_K))
    route_weights = jnp.clip(0.2 + 0.8 * jax.random.uniform(key_list[23], (TOKEN_TOTAL, TOP_K), jnp.float32) ** block_levels(key_list[23], (TOKEN_TOTAL, TOP_K), ((0, 16),), -0.2, 0.2), 0.2, 1.0)
    return dict(tokens=tokens, state=state, w_recep=w_recep, w_key=w_key, w_value=w_value, w_out=w_out, decay_base=decay_base, decay_down=decay_down, decay_up=decay_up, rate_base=rate_base, rate_down=rate_down, rate_up=rate_up, head_gain=head_gain, first_gain=first_gain, expert_gate=expert_gate, expert_up=expert_up, expert_down=expert_down, dense_gate=dense_gate, dense_up=dense_up, dense_down=dense_down, branch_gate=branch_gate, second_gain=second_gain, routes=routes, route_weights=route_weights)


residual_scale = 1.4142135623730951
norm_epsilon = 1e-05
head_epsilon = 0.00064
key_epsilon = 1e-06

def time_mixer(tokens, state, w_recep, w_key, w_value, w_out, decay_base, decay_down, decay_up, rate_base, rate_down, rate_up, head_gain):
    row_count = tokens.shape[0]
    head_count = state.shape[1]
    head_size = state.shape[3]
    recep = jnp.dot(tokens, w_recep, preferred_element_type=jnp.float32).reshape(row_count, head_count, head_size)
    key_vecs = jnp.dot(tokens, w_key, preferred_element_type=jnp.float32).reshape(row_count, head_count, head_size)
    value_vecs = jnp.dot(tokens, w_value, preferred_element_type=jnp.float32).reshape(row_count, head_count, head_size)
    decay_low = jnp.tanh(jnp.dot(tokens, decay_down, preferred_element_type=jnp.float32)).astype(jnp.bfloat16)
    decay_pre = decay_base + jnp.dot(decay_low, decay_up, preferred_element_type=jnp.float32)
    log_rate = -jax.nn.softplus(-decay_pre) - 0.5
    decay = jnp.exp(-jnp.exp(log_rate)).reshape(row_count, head_count, head_size)
    rate_low = jnp.dot(tokens, rate_down, preferred_element_type=jnp.float32).astype(jnp.bfloat16)
    in_rate = jax.nn.sigmoid(rate_base + jnp.dot(rate_low, rate_up, preferred_element_type=jnp.float32)).reshape(row_count, head_count, head_size)
    unit_keys = key_vecs * lax.rsqrt(lax.optimization_barrier(jnp.sum(key_vecs * key_vecs, -1, keepdims=True)) + key_epsilon)
    removed = jnp.einsum('bhij,bhj->bhi', state, -unit_keys)
    updated = state * decay[:, :, None, :] + removed[..., None] * (unit_keys * in_rate)[:, :, None, :] + value_vecs[..., None] * key_vecs[:, :, None, :]
    read_out = jnp.einsum('bhij,bhj->bhi', updated, recep)
    centre = lax.optimization_barrier(jnp.mean(read_out, -1, keepdims=True))
    spread = lax.optimization_barrier(jnp.mean(jnp.square(read_out - centre), -1, keepdims=True))
    normed = ((read_out - centre) * lax.rsqrt(spread + head_epsilon)).reshape(row_count, head_count * head_size) * head_gain
    return jnp.dot(normed.astype(jnp.bfloat16), w_out, preferred_element_type=jnp.float32)

def first_norm(values, gain):
    centre = lax.optimization_barrier(jnp.mean(values, -1, keepdims=True))
    spread = lax.optimization_barrier(jnp.mean(jnp.square(values - centre), -1, keepdims=True))
    return ((values - centre) * lax.rsqrt(spread + norm_epsilon) * gain).astype(jnp.bfloat16)

def route_tables(routes, route_weights, experts, capacity):
    expert_hits = (routes[:, :, None] == jnp.arange(experts, dtype=jnp.int32)[None, None, :]).astype(jnp.int32)
    row_hits = lax.optimization_barrier(jnp.sum(expert_hits, 1, dtype=jnp.int32))
    earlier = jnp.cumsum(row_hits, 0, dtype=jnp.int32) - row_hits
    slot_index = lax.optimization_barrier(jnp.sum(earlier[:, None, :] * expert_hits, 2, dtype=jnp.int32))
    target = routes * capacity + slot_index
    places = jnp.arange(experts * capacity, dtype=jnp.int32)
    slot_match = target[:, :, None] == places[None, None, :]
    dispatch_tokens = jnp.any(slot_match, 1).astype(jnp.bfloat16)
    combine_experts = lax.optimization_barrier(jnp.sum(jnp.where(slot_match, route_weights[:, :, None], 0.0), 1))
    return (dispatch_tokens, combine_experts)

def one_expert(operands):
    rows_in, gate_all, up_all, down_all = operands
    gate_pre = jnp.dot(rows_in, gate_all, preferred_element_type=jnp.float32)
    up_pre = jnp.dot(rows_in, up_all, preferred_element_type=jnp.float32)
    hidden = (jax.nn.silu(gate_pre) * up_pre).astype(jnp.bfloat16)
    return jnp.dot(hidden, down_all, preferred_element_type=jnp.float32)

def reference(tokens, state, w_recep, w_key, w_value, w_out, decay_base, decay_down, decay_up, rate_base, rate_down, rate_up, head_gain, first_gain, expert_gate, expert_up, expert_down, dense_gate, dense_up, dense_down, branch_gate, second_gain, routes, route_weights):
    mixed = time_mixer(tokens, state, w_recep, w_key, w_value, w_out, decay_base, decay_down, decay_up, rate_base, rate_down, rate_up, head_gain)
    x_mid = first_norm(residual_scale * tokens.astype(jnp.float32) + mixed, first_gain)
    route_blocks = routes.reshape(N_EP, B_DEV, TOP_K)
    weight_blocks = route_weights.reshape(N_EP, B_DEV, TOP_K)
    dispatch_tokens, combine_experts = jax.vmap(partial(route_tables, experts=EXPERTS, capacity=CAP))(route_blocks, weight_blocks)
    token_block_rows = x_mid.reshape(N_EP, B_DEV, MODEL_DIMENSION).astype(jnp.float32)
    packed_rows = jnp.einsum('ekc,ekq->ecq', dispatch_tokens.astype(jnp.float32), token_block_rows).astype(jnp.bfloat16)
    expert_rows = packed_rows.reshape(N_EP, EXPERTS, CAP, MODEL_DIMENSION).transpose(1, 0, 2, 3).reshape(EXPERTS, N_EP * CAP, MODEL_DIMENSION)
    gate_all = expert_gate.reshape(EXPERTS, SPLIT, MODEL_DIMENSION, FF_E // SPLIT).transpose(0, 2, 1, 3).reshape(EXPERTS, MODEL_DIMENSION, FF_E)
    up_all = expert_up.reshape(EXPERTS, SPLIT, MODEL_DIMENSION, FF_E // SPLIT).transpose(0, 2, 1, 3).reshape(EXPERTS, MODEL_DIMENSION, FF_E)
    down_all = expert_down.reshape(EXPERTS, FF_E, MODEL_DIMENSION)
    produced = lax.map(one_expert, (expert_rows, gate_all, up_all, down_all))
    returned_rows = produced.reshape(EXPERTS, N_EP, CAP, MODEL_DIMENSION).transpose(1, 0, 2, 3).reshape(N_EP, EXPERTS * CAP, MODEL_DIMENSION)
    routed_tokens = jnp.einsum('lhs,lsu->lhu', combine_experts, returned_rows, precision=lax.Precision.HIGHEST).reshape(TOKEN_TOTAL, MODEL_DIMENSION)
    gate_pre = lax.dot_general(x_mid, dense_gate, (((1,), (1,)), ((), ())), preferred_element_type=jnp.float32)
    up_pre = lax.dot_general(x_mid, dense_up, (((1,), (1,)), ((), ())), preferred_element_type=jnp.float32)
    dense_hidden = (jax.nn.silu(gate_pre) * up_pre).astype(jnp.bfloat16)
    dense_part = jnp.dot(dense_hidden, dense_down, preferred_element_type=jnp.float32)
    branch = jax.nn.sigmoid(jnp.dot(x_mid, branch_gate, preferred_element_type=jnp.float32))
    second_sum = residual_scale * x_mid.astype(jnp.float32) + routed_tokens + branch[:, None] * dense_part
    average = lax.optimization_barrier(jnp.mean(second_sum, 1))
    square_mean = lax.optimization_barrier(jnp.mean(second_sum * second_sum, 1))
    spread = square_mean - average * average
    return ((second_sum - average[:, None]) * lax.rsqrt(spread + norm_epsilon)[:, None] * second_gain).astype(jnp.bfloat16)
```

```python
import functools

import jax
import jax.numpy as jnp
from jax import lax
from jax.experimental import pallas as pl
from jax.experimental.pallas import tpu as pltpu
from jax.sharding import PartitionSpec as P

SPLIT = 4
CORES = 2
LANES = 128

residual_scale = 1.4142135623730951
norm_epsilon = 1e-05
head_epsilon = 0.00064
key_epsilon = 1e-06
decay_scale = 0.6065306597126334

F32 = jnp.float32
BF16 = jnp.bfloat16
MESH = pl.DeviceIdType.MESH
NT = (((1,), (1,)), ((), ()))


def dot(a, b):
    return jnp.dot(a, b, preferred_element_type=F32)


def dot_nt(a, b):
    return lax.dot_general(a, b, NT, preferred_element_type=F32)


def layer_kernel(
    ep,
    tp,
    tokens,
    decay_base,
    rate_base,
    head_gain,
    first_gain,
    branch_gate,
    second_gain,
    routes,
    route_weights,
    state_h,
    w_recep_h,
    w_key_h,
    w_value_h,
    w_out_h,
    decay_down_h,
    decay_up_h,
    rate_down_h,
    rate_up_h,
    gate_h,
    up_h,
    down_h,
    dgate_h,
    dup_h,
    ddown_h,
    out,
    state,
    w_recep,
    w_key,
    w_value,
    w_out,
    decay_down,
    decay_up,
    rate_down,
    rate_up,
    gate,
    up,
    down,
    dgate,
    dup,
    ddown,
    mix_send,
    mix_recv,
    xall,
    core_send,
    core_recv,
    plane_send,
    plane_recv,
    line_send,
    line_recv,
    stat_send,
    stat_recv,
    load_sem,
    mix_sems,
    zag_sems,
    xag_sems,
    cag_sems,
    core_sems,
    plane_sems,
    line_sems,
    stat_sems,
):
    rows, width = tokens.shape
    quarter = w_recep.shape[1]
    heads, size = state.shape[1], state.shape[3]
    side = tp
    layers = ep // (side * CORES)
    plane = tp * side
    experts = ep // SPLIT

    me = lax.axis_index("ep")
    mt = lax.axis_index("tp")
    mc = me % CORES
    mx = (me // CORES) % side
    mz = me // (CORES * side)

    def at(z, x, c):
        return (z * side + x) * CORES + c

    pairs = (
        (w_key_h, w_key),
        (decay_down_h, decay_down),
        (rate_down_h, rate_down),
        (decay_up_h, decay_up),
        (rate_up_h, rate_up),
        (w_recep_h, w_recep),
        (w_value_h, w_value),
        (state_h, state),
        (w_out_h, w_out),
        (gate_h, gate),
        (up_h, up),
        (dgate_h, dgate),
        (dup_h, dup),
        (down_h, down),
        (ddown_h, ddown),
    )
    loads = {}
    for n, (src, dst) in enumerate(pairs):
        copy = pltpu.make_async_copy(src, dst, load_sem.at[n])
        copy.start()
        loads[n] = copy

    def peer(e, t):
        return {"ep": e, "tp": t}

    greeted = []
    for d in range(1, layers):
        greeted.append(peer(at((mz + d) % layers, mx, mc), mt))
    for d in range(1, plane):
        m = (mt * side + mx + d) % plane
        greeted.append(peer(at(mz, m % side, mc), m // side))
    greeted.append(peer(at(mz, mx, 1 - mc), mt))
    barrier = pltpu.get_barrier_semaphore()
    for who in greeted:
        pl.semaphore_signal(barrier, inc=1, device_id=who, device_id_type=MESH)

    sent = []

    def send(src, dst, sems, who):
        copy = pltpu.make_async_remote_copy(
            src_ref=src,
            dst_ref=dst,
            send_sem=sems.at[0],
            recv_sem=sems.at[1],
            device_id=who,
            device_id_type=MESH,
        )
        copy.start()
        sent.append(copy)
        return copy

    tok = tokens[...]
    loads[0].wait()
    key_all = dot(tok, w_key[...])
    for n in (1, 2, 3, 4):
        loads[n].wait()
    decay_low = jnp.tanh(dot_nt(tok, decay_down[...])).astype(BF16)
    decay_pre = decay_base[...] + dot(decay_low, decay_up[...])
    decay_all = jnp.exp(-decay_scale * jax.nn.sigmoid(decay_pre))
    rate_low = dot_nt(tok, rate_down[...]).astype(BF16)
    rate_all = jax.nn.sigmoid(rate_base[...] + dot(rate_low, rate_up[...]))
    loads[5].wait()
    recep_all = dot(tok, w_recep[...])
    loads[6].wait()
    value_all = dot(tok, w_value[...])
    loads[7].wait()
    per = LANES // size
    row_id = lax.broadcasted_iota(jnp.int32, (2 * rows, LANES), 0) % rows
    lane_tok = lax.broadcasted_iota(jnp.int32, (2 * rows, LANES), 1) // size
    normed = []
    for h in range(heads):
        cut = slice(h * size, (h + 1) * size)
        k = key_all[:, cut]
        r = recep_all[:, cut]
        v = value_all[:, cut]
        unit = k * lax.rsqrt(jnp.sum(k * k, -1, keepdims=True) + key_epsilon)
        probe = jnp.concatenate([unit, decay_all[:, cut] * r], 0).astype(BF16)
        block = state[:, h].reshape(rows * size, size).astype(BF16)
        cross = dot_nt(probe, block)
        folded = jnp.zeros((2 * rows, LANES), F32)
        for g in range(rows * size // LANES):
            part = cross[:, g * LANES : (g + 1) * LANES]
            folded = folded + jnp.where(row_id == g * per + lane_tok, part, 0.0)
        own = folded[:, :size]
        for g in range(1, per):
            own = own + folded[:, g * size : (g + 1) * size]
        c1 = jnp.sum(unit * rate_all[:, cut] * r, -1, keepdims=True)
        c2 = jnp.sum(k * r, -1, keepdims=True)
        read = own[rows:] - own[:rows] * c1 + v * c2
        read = read - jnp.mean(read, -1, keepdims=True)
        spread = jnp.mean(read * read, -1, keepdims=True)
        normed.append(read * lax.rsqrt(spread + head_epsilon))
    head_out = (jnp.concatenate(normed, 1) * head_gain[...]).astype(BF16)
    loads[8].wait()
    mix_send[...] = dot(head_out, w_out[...]).astype(BF16)

    pl.semaphore_wait(barrier, len(greeted))
    copies = []
    for d in range(1, tp):
        copies.append(
            send(mix_send, mix_recv.at[d - 1], mix_sems.at[d - 1], peer(me, (mt + d) % tp))
        )

    half = LANES // 2
    lane = lax.broadcasted_iota(jnp.int32, (rows, LANES), 1)
    names = routes[...]
    weights = route_weights[...]
    place = lax.broadcasted_iota(jnp.int32, (LANES, rows), 0)
    spots = jnp.zeros((LANES, rows), F32)
    for k in range(names.shape[0]):
        spots = spots + jnp.where(place % half == names[k : k + 1], weights[k : k + 1], 0.0)
    high = spots.astype(BF16).astype(F32)
    spots = jnp.where(place < half, high, spots - high).astype(BF16)
    one = lax.broadcasted_iota(jnp.int32, (rows, rows), 0) == lax.broadcasted_iota(
        jnp.int32, (rows, rows), 1
    )
    extra = dot_nt(jnp.where(one, 1.0, 0.0).astype(BF16), spots)

    total = residual_scale * tok.astype(F32) + mix_send[...].astype(F32)
    for d in range(1, tp):
        copies[d - 1].wait_recv()
        total = total + mix_recv[d - 1].astype(F32)
    total = total - jnp.mean(total, -1, keepdims=True)
    spread = jnp.mean(total * total, -1, keepdims=True)
    x_mid = (total * lax.rsqrt(spread + norm_epsilon) * first_gain[...]).astype(BF16)
    branch = jax.nn.sigmoid(
        jnp.sum(x_mid.astype(F32) * branch_gate[...].astype(F32).reshape(1, width), -1, keepdims=True)
    )
    high = branch.astype(BF16).astype(F32)
    extra = jnp.where(lane == experts, high, extra)
    extra = jnp.where(lane == half + experts, branch - high, extra).astype(BF16)
    xall[me, :, :width] = x_mid
    xall[me, :, width:] = extra

    def gather_wait(kind, d, n):
        sems = {"z": zag_sems, "x": xag_sems, "c": cag_sems}[kind]
        sem = sems.at[d - 1] if kind == "z" else sems.at[d, n]
        pltpu.make_async_remote_copy(
            src_ref=xall.at[me],
            dst_ref=xall.at[me],
            send_sem=sem.at[0],
            recv_sem=sem.at[1],
            device_id=peer(at(mz, mx, 1 - mc), mt),
            device_id_type=MESH,
        ).wait_recv()

    for d in range(1, layers):
        send(
            xall.at[me],
            xall.at[me],
            zag_sems.at[d - 1],
            peer(at((mz + d) % layers, mx, mc), mt),
        )

    def forward_line(d):
        b = at((mz + layers - d) % layers, mx, mc)
        if d:
            gather_wait("z", d, 0)
        for n in range(1, side):
            send(
                xall.at[b],
                xall.at[b],
                xag_sems.at[d, n - 1],
                peer(at(mz, (mx + n) % side, mc), mt),
            )
        send(xall.at[b], xall.at[b], cag_sems.at[d, 0], peer(at(mz, mx, 1 - mc), mt))

    def forward_side(d):
        for n in range(1, side):
            b = at((mz + layers - d) % layers, (mx + side - n) % side, mc)
            gather_wait("x", d, n - 1)
            send(xall.at[b], xall.at[b], cag_sems.at[d, n], peer(at(mz, mx, 1 - mc), mt))

    for d in range(layers):
        forward_line(d)
        if d:
            forward_side(d - 1)
    forward_side(layers - 1)

    count = side * CORES * rows
    expert = me // SPLIT
    lane_c = lax.broadcasted_iota(jnp.int32, (count, LANES), 1) % half

    def compute(d):
        z = (mz + layers - d) % layers
        first = at(z, 0, 0)
        for n in range(side):
            gather_wait("c", d, n)
        if d == 0:
            for n in range(9, 15):
                loads[n].wait()
        blocks = xall[pl.ds(first, side * CORES), :, :]
        flat = blocks.reshape(count, width + LANES)
        x = flat[:, :width]
        tail = flat[:, width:].astype(F32)
        weight = jnp.sum(jnp.where(lane_c == expert, tail, 0.0), -1, keepdims=True)
        branch_c = jnp.sum(jnp.where(lane_c == experts, tail, 0.0), -1, keepdims=True)
        hidden = (jax.nn.silu(dot_nt(x, gate[...])) * dot_nt(x, up[...])).astype(BF16)
        dense = (jax.nn.silu(dot_nt(x, dgate[...])) * dot_nt(x, dup[...])).astype(BF16)
        dense_out = dot(dense, ddown[...]) * branch_c
        for q in range(tp):
            part = dot(hidden, down[:, q * quarter : (q + 1) * quarter]) * weight
            part = part + jnp.where(mt == q, dense_out, 0.0)
            part = part.astype(BF16).reshape(side, CORES, rows, quarter)
            for x_to in range(side):
                for c_to in range(CORES):
                    core_send[d, c_to, q * side + x_to] = part[x_to, c_to]
        return send(
            core_send.at[d, 1 - mc],
            core_recv.at[d],
            core_sems.at[d],
            peer(at(mz, mx, 1 - mc), mt),
        )

    def plane_step(d, copy):
        copy.wait_recv()
        plane_send[d] = (core_send[d, mc].astype(F32) + core_recv[d].astype(F32)).astype(BF16)
        out_copies = []
        for n in range(1, plane):
            m = (mt * side + mx + n) % plane
            out_copies.append(
                send(
                    plane_send.at[d, m],
                    plane_recv.at[d, n - 1],
                    plane_sems.at[d, n - 1],
                    peer(at(mz, m % side, mc), m // side),
                )
            )
        return out_copies

    def line_step(d, in_copies):
        acc = plane_send[d, mt * side + mx].astype(F32)
        for n in range(1, plane):
            in_copies[n - 1].wait_recv()
            acc = acc + plane_recv[d, n - 1].astype(F32)
        if d == 0:
            return acc
        line_send[d - 1] = acc.astype(BF16)
        return send(
            line_send.at[d - 1],
            line_recv.at[d - 1],
            line_sems.at[d - 1],
            peer(at((mz + layers - d) % layers, mx, mc), mt),
        )

    core_out, plane_out, line_out = {}, {}, {}
    for d in range(layers + 2):
        if d < layers:
            core_out[d] = compute(d)
        if 0 <= d - 1 < layers:
            plane_out[d - 1] = plane_step(d - 1, core_out[d - 1])
        if 0 <= d - 2 < layers:
            line_out[d - 2] = line_step(d - 2, plane_out[d - 2])

    columns = pl.ds(pl.multiple_of(mt * quarter, quarter), quarter)
    second = residual_scale * xall[me, :, columns].astype(F32) + line_out[0]
    for d in range(1, layers):
        line_out[d].wait_recv()
        second = second + line_recv[d - 1].astype(F32)

    stat = jnp.where(
        lane == 0,
        jnp.sum(second, -1, keepdims=True),
        jnp.where(lane == 1, jnp.sum(second * second, -1, keepdims=True), 0.0),
    )
    stat_send[...] = stat
    copies = []
    for d in range(1, tp):
        copies.append(
            send(stat_send, stat_recv.at[d - 1], stat_sems.at[d - 1], peer(me, (mt + d) % tp))
        )
    for d in range(1, tp):
        copies[d - 1].wait_recv()
        stat = stat + stat_recv[d - 1]
    average = stat[:, 0:1] / width
    spread = stat[:, 1:2] / width - average * average
    out[...] = (
        (second - average) * lax.rsqrt(spread + norm_epsilon) * second_gain[...]
    ).astype(BF16)
    for copy in sent:
        copy.wait_send()


def shards(
    tokens,
    state,
    w_recep,
    w_key,
    w_value,
    w_out,
    decay_base,
    decay_down,
    decay_up,
    rate_base,
    rate_down,
    rate_up,
    head_gain,
    first_gain,
    expert_gate,
    expert_up,
    expert_down,
    dense_gate,
    dense_up,
    dense_down,
    branch_gate,
    second_gain,
    routes,
    route_weights,
):
    ep, tp = lax.axis_size("ep"), lax.axis_size("tp")
    rows, width = tokens.shape
    quarter = w_recep.shape[1]
    side = tp
    layers = ep // (side * CORES)
    plane = tp * side
    large = (
        state,
        w_recep,
        w_key,
        w_value,
        w_out,
        decay_down.T,
        decay_up,
        rate_down.T,
        rate_up,
        expert_gate[0].T,
        expert_up[0].T,
        expert_down[0],
        dense_gate,
        dense_up,
        dense_down,
    )
    small = (
        tokens,
        decay_base[None],
        rate_base[None],
        head_gain[None],
        first_gain[None],
        branch_gate,
        second_gain[None],
        routes.T,
        route_weights.T,
    )
    dma = pltpu.SemaphoreType.DMA
    return pl.pallas_call(
        functools.partial(layer_kernel, ep, tp),
        out_shape=jax.ShapeDtypeStruct((rows, quarter), BF16),
        in_specs=[pl.BlockSpec(memory_space=pltpu.VMEM)] * len(small)
        + [pl.BlockSpec(memory_space=pl.ANY)] * len(large),
        out_specs=pl.BlockSpec(memory_space=pltpu.VMEM),
        scratch_shapes=[pltpu.VMEM(a.shape, a.dtype) for a in large]
        + [
            pltpu.VMEM((rows, width), BF16),
            pltpu.VMEM((tp - 1, rows, width), BF16),
            pltpu.VMEM((ep, rows, width + LANES), BF16),
            pltpu.VMEM((layers, CORES, plane, rows, quarter), BF16),
            pltpu.VMEM((layers, plane, rows, quarter), BF16),
            pltpu.VMEM((layers, plane, rows, quarter), BF16),
            pltpu.VMEM((layers, plane - 1, rows, quarter), BF16),
            pltpu.VMEM((layers - 1, rows, quarter), BF16),
            pltpu.VMEM((layers - 1, rows, quarter), BF16),
            pltpu.VMEM((rows, LANES), F32),
            pltpu.VMEM((tp - 1, rows, LANES), F32),
            dma((len(large),)),
            dma((tp - 1, 2)),
            dma((layers - 1, 2)),
            dma((layers, side - 1, 2)),
            dma((layers, side, 2)),
            dma((layers, 2)),
            dma((layers, plane - 1, 2)),
            dma((layers - 1, 2)),
            dma((tp - 1, 2)),
        ],
        compiler_params=pltpu.CompilerParams(collective_id=0, has_side_effects=True),
    )(*small, *large)


def solution(mesh):
    return jax.shard_map(
        shards,
        mesh=mesh,
        in_specs=(
            P("ep", None),
            P("ep", "tp", None, None),
            P(None, "tp"),
            P(None, "tp"),
            P(None, "tp"),
            P("tp", None),
            P("tp"),
            P(),
            P(None, "tp"),
            P("tp"),
            P(),
            P(None, "tp"),
            P("tp"),
            P(),
            P("ep", None, "tp"),
            P("ep", None, "tp"),
            P("ep", "tp", None),
            P("ep", None),
            P("ep", None),
            P("ep", "tp"),
            P(),
            P("tp"),
            P("ep", None),
            P("ep", None),
        ),
        out_specs=P("ep", "tp"),
        check_vma=False,
    )
```

```python
import functools

import jax
import jax.numpy as jnp
from jax import lax
from jax.experimental import pallas as pl
from jax.experimental.pallas import tpu as pltpu
from jax.sharding import PartitionSpec as P

SPLIT = 4
CORES = 2
LANES = 128

residual_scale = 1.4142135623730951
norm_epsilon = 1e-05
head_epsilon = 0.00064
key_epsilon = 1e-06
decay_scale = 0.6065306597126334

F32 = jnp.float32
BF16 = jnp.bfloat16
MESH = pl.DeviceIdType.MESH
NT = (((1,), (1,)), ((), ()))


def dot(a, b):
    return jnp.dot(a, b, preferred_element_type=F32)


def dot_nt(a, b):
    return lax.dot_general(a, b, NT, preferred_element_type=F32)


def layer_kernel(
    ep,
    tp,
    tokens,
    decay_base,
    rate_base,
    head_gain,
    first_gain,
    branch_gate,
    second_gain,
    routes,
    route_weights,
    state_h,
    w_recep_h,
    w_key_h,
    w_value_h,
    w_out_h,
    decay_down_h,
    decay_up_h,
    rate_down_h,
    rate_up_h,
    gate_h,
    up_h,
    down_h,
    dgate_h,
    dup_h,
    ddown_h,
    out,
    state,
    w_recep,
    w_key,
    w_value,
    w_out,
    decay_down,
    decay_up,
    rate_down,
    rate_up,
    gate,
    up,
    down,
    dgate,
    dup,
    ddown,
    mix_send,
    mix_recv,
    xall,
    core_send,
    core_recv,
    plane_send,
    plane_recv,
    line_send,
    line_recv,
    stat_send,
    stat_recv,
    load_sem,
    mix_sems,
    zag_sems,
    xag_sems,
    cag_sems,
    core_sems,
    plane_sems,
    line_sems,
    stat_sems,
):
    rows, width = tokens.shape
    quarter = w_recep.shape[1]
    heads, size = state.shape[1], state.shape[3]
    side = tp
    layers = ep // (side * CORES)
    plane = tp * side
    experts = ep // SPLIT

    me = lax.axis_index("ep")
    mt = lax.axis_index("tp")
    mc = me % CORES
    mx = (me // CORES) % side
    mz = me // (CORES * side)

    def at(z, x, c):
        return (z * side + x) * CORES + c

    pairs = (
        (w_key_h, w_key),
        (decay_down_h, decay_down),
        (rate_down_h, rate_down),
        (decay_up_h, decay_up),
        (rate_up_h, rate_up),
        (w_recep_h, w_recep),
        (w_value_h, w_value),
        (state_h, state),
        (w_out_h, w_out),
        (gate_h, gate),
        (up_h, up),
        (dgate_h, dgate),
        (dup_h, dup),
        (down_h, down),
        (ddown_h, ddown),
    )
    loads = {}
    for n, (src, dst) in enumerate(pairs):
        copy = pltpu.make_async_copy(src, dst, load_sem.at[n])
        copy.start()
        loads[n] = copy

    def peer(e, t):
        return {"ep": e, "tp": t}

    greeted = []
    for d in range(1, layers):
        greeted.append(peer(at((mz + d) % layers, mx, mc), mt))
    for d in range(1, plane):
        m = (mt * side + mx + d) % plane
        greeted.append(peer(at(mz, m % side, mc), m // side))
    greeted.append(peer(at(mz, mx, 1 - mc), mt))
    barrier = pltpu.get_barrier_semaphore()
    for who in greeted:
        pl.semaphore_signal(barrier, inc=1, device_id=who, device_id_type=MESH)

    sent = []

    def send(src, dst, sems, who):
        copy = pltpu.make_async_remote_copy(
            src_ref=src,
            dst_ref=dst,
            send_sem=sems.at[0],
            recv_sem=sems.at[1],
            device_id=who,
            device_id_type=MESH,
        )
        copy.start()
        sent.append(copy)
        return copy

    tok = tokens[...]
    loads[0].wait()
    key_all = dot(tok, w_key[...])
    for n in (1, 2, 3, 4):
        loads[n].wait()
    decay_low = jnp.tanh(dot_nt(tok, decay_down[...])).astype(BF16)
    decay_pre = decay_base[...] + dot(decay_low, decay_up[...])
    decay_all = jnp.exp(-decay_scale * jax.nn.sigmoid(decay_pre))
    rate_low = dot_nt(tok, rate_down[...]).astype(BF16)
    rate_all = jax.nn.sigmoid(rate_base[...] + dot(rate_low, rate_up[...]))
    loads[5].wait()
    recep_all = dot(tok, w_recep[...])
    loads[6].wait()
    value_all = dot(tok, w_value[...])
    loads[7].wait()
    per = LANES // size
    row_id = lax.broadcasted_iota(jnp.int32, (2 * rows, LANES), 0) % rows
    lane_tok = lax.broadcasted_iota(jnp.int32, (2 * rows, LANES), 1) // size
    normed = []
    for h in range(heads):
        cut = slice(h * size, (h + 1) * size)
        k = key_all[:, cut]
        r = recep_all[:, cut]
        v = value_all[:, cut]
        unit = k * lax.rsqrt(jnp.sum(k * k, -1, keepdims=True) + key_epsilon)
        probe = jnp.concatenate([unit, decay_all[:, cut] * r], 0).astype(BF16)
        block = state[:, h].reshape(rows * size, size).astype(BF16)
        cross = dot_nt(probe, block)
        folded = jnp.zeros((2 * rows, LANES), F32)
        for g in range(rows * size // LANES):
            part = cross[:, g * LANES : (g + 1) * LANES]
            folded = folded + jnp.where(row_id == g * per + lane_tok, part, 0.0)
        own = folded[:, :size]
        for g in range(1, per):
            own = own + folded[:, g * size : (g + 1) * size]
        c1 = jnp.sum(unit * rate_all[:, cut] * r, -1, keepdims=True)
        c2 = jnp.sum(k * r, -1, keepdims=True)
        read = own[rows:] - own[:rows] * c1 + v * c2
        read = read - jnp.mean(read, -1, keepdims=True)
        spread = jnp.mean(read * read, -1, keepdims=True)
        normed.append(read * lax.rsqrt(spread + head_epsilon))
    head_out = (jnp.concatenate(normed, 1) * head_gain[...]).astype(BF16)
    loads[8].wait()
    mix_send[...] = dot(head_out, w_out[...]).astype(BF16)

    pl.semaphore_wait(barrier, len(greeted))
    copies = []
    for d in range(1, tp):
        copies.append(
            send(mix_send, mix_recv.at[d - 1], mix_sems.at[d - 1], peer(me, (mt + d) % tp))
        )

    half = LANES // 2
    lane = lax.broadcasted_iota(jnp.int32, (rows, LANES), 1)
    names = routes[...]
    weights = route_weights[...]
    place = lax.broadcasted_iota(jnp.int32, (LANES, rows), 0)
    spots = jnp.zeros((LANES, rows), F32)
    for k in range(names.shape[0]):
        spots = spots + jnp.where(place % half == names[k : k + 1], weights[k : k + 1], 0.0)
    high = spots.astype(BF16).astype(F32)
    spots = jnp.where(place < half, high, spots - high).astype(BF16)
    one = lax.broadcasted_iota(jnp.int32, (rows, rows), 0) == lax.broadcasted_iota(
        jnp.int32, (rows, rows), 1
    )
    extra = dot_nt(jnp.where(one, 1.0, 0.0).astype(BF16), spots)

    total = residual_scale * tok.astype(F32) + mix_send[...].astype(F32)
    for d in range(1, tp):
        copies[d - 1].wait_recv()
        total = total + mix_recv[d - 1].astype(F32)
    total = total - jnp.mean(total, -1, keepdims=True)
    spread = jnp.mean(total * total, -1, keepdims=True)
    x_mid = (total * lax.rsqrt(spread + norm_epsilon) * first_gain[...]).astype(BF16)
    branch = jax.nn.sigmoid(
        jnp.sum(x_mid.astype(F32) * branch_gate[...].astype(F32).reshape(1, width), -1, keepdims=True)
    )
    high = branch.astype(BF16).astype(F32)
    extra = jnp.where(lane == experts, high, extra)
    extra = jnp.where(lane == half + experts, branch - high, extra).astype(BF16)
    xall[me, :, :width] = x_mid
    xall[me, :, width:] = extra

    def gather_wait(kind, d, n):
        sems = {"z": zag_sems, "x": xag_sems, "c": cag_sems}[kind]
        sem = sems.at[d - 1] if kind == "z" else sems.at[d, n]
        pltpu.make_async_remote_copy(
            src_ref=xall.at[me],
            dst_ref=xall.at[me],
            send_sem=sem.at[0],
            recv_sem=sem.at[1],
            device_id=peer(at(mz, mx, 1 - mc), mt),
            device_id_type=MESH,
        ).wait_recv()

    for d in range(1, layers):
        send(
            xall.at[me],
            xall.at[me],
            zag_sems.at[d - 1],
            peer(at((mz + d) % layers, mx, mc), mt),
        )

    def forward_line(d):
        b = at((mz + layers - d) % layers, mx, mc)
        if d:
            gather_wait("z", d, 0)
        for n in range(1, side):
            send(
                xall.at[b],
                xall.at[b],
                xag_sems.at[d, n - 1],
                peer(at(mz, (mx + n) % side, mc), mt),
            )
        send(xall.at[b], xall.at[b], cag_sems.at[d, 0], peer(at(mz, mx, 1 - mc), mt))

    def forward_side(d):
        for n in range(1, side):
            b = at((mz + layers - d) % layers, (mx + side - n) % side, mc)
            gather_wait("x", d, n - 1)
            send(xall.at[b], xall.at[b], cag_sems.at[d, n], peer(at(mz, mx, 1 - mc), mt))

    count = side * CORES * rows
    expert = me // SPLIT
    lane_c = lax.broadcasted_iota(jnp.int32, (count, LANES), 1) % half

    def compute(d):
        z = (mz + layers - d) % layers
        first = at(z, 0, 0)
        for n in range(side):
            gather_wait("c", d, n)
        if d == 0:
            for n in range(9, 15):
                loads[n].wait()
        blocks = xall[pl.ds(first, side * CORES), :, :]
        flat = blocks.reshape(count, width + LANES)
        x = flat[:, :width]
        tail = flat[:, width:].astype(F32)
        weight = jnp.sum(jnp.where(lane_c == expert, tail, 0.0), -1, keepdims=True)
        branch_c = jnp.sum(jnp.where(lane_c == experts, tail, 0.0), -1, keepdims=True)
        hidden = (jax.nn.silu(dot_nt(x, gate[...])) * dot_nt(x, up[...])).astype(BF16)
        dense = (jax.nn.silu(dot_nt(x, dgate[...])) * dot_nt(x, dup[...])).astype(BF16)
        dense_out = dot(dense, ddown[...]) * branch_c
        for q in range(tp):
            part = dot(hidden, down[:, q * quarter : (q + 1) * quarter]) * weight
            part = part + jnp.where(mt == q, dense_out, 0.0)
            part = part.astype(BF16).reshape(side, CORES, rows, quarter)
            for x_to in range(side):
                for c_to in range(CORES):
                    core_send[d, c_to, q * side + x_to] = part[x_to, c_to]
        return send(
            core_send.at[d, 1 - mc],
            core_recv.at[d],
            core_sems.at[d],
            peer(at(mz, mx, 1 - mc), mt),
        )

    def plane_step(d, copy):
        copy.wait_recv()
        plane_send[d] = (core_send[d, mc].astype(F32) + core_recv[d].astype(F32)).astype(BF16)
        out_copies = []
        for n in range(1, plane):
            m = (mt * side + mx + n) % plane
            out_copies.append(
                send(
                    plane_send.at[d, m],
                    plane_recv.at[d, n - 1],
                    plane_sems.at[d, n - 1],
                    peer(at(mz, m % side, mc), m // side),
                )
            )
        return out_copies

    def line_step(d, in_copies):
        acc = plane_send[d, mt * side + mx].astype(F32)
        for n in range(1, plane):
            in_copies[n - 1].wait_recv()
            acc = acc + plane_recv[d, n - 1].astype(F32)
        if d == 0:
            return acc
        line_send[d - 1] = acc.astype(BF16)
        return send(
            line_send.at[d - 1],
            line_recv.at[d - 1],
            line_sems.at[d - 1],
            peer(at((mz + layers - d) % layers, mx, mc), mt),
        )

    core_out, plane_out, line_out = {}, {}, {}
    for d in range(layers + 4):
        if d < layers:
            forward_line(d)
        if 0 <= d - 1 < layers:
            forward_side(d - 1)
        if 0 <= d - 2 < layers:
            core_out[d - 2] = compute(d - 2)
        if 0 <= d - 3 < layers:
            plane_out[d - 3] = plane_step(d - 3, core_out[d - 3])
        if 0 <= d - 4 < layers:
            line_out[d - 4] = line_step(d - 4, plane_out[d - 4])

    columns = pl.ds(pl.multiple_of(mt * quarter, quarter), quarter)
    second = residual_scale * xall[me, :, columns].astype(F32) + line_out[0]
    for d in range(1, layers):
        line_out[d].wait_recv()
        second = second + line_recv[d - 1].astype(F32)

    stat = jnp.where(
        lane == 0,
        jnp.sum(second, -1, keepdims=True),
        jnp.where(lane == 1, jnp.sum(second * second, -1, keepdims=True), 0.0),
    )
    stat_send[...] = stat
    copies = []
    for d in range(1, tp):
        copies.append(
            send(stat_send, stat_recv.at[d - 1], stat_sems.at[d - 1], peer(me, (mt + d) % tp))
        )
    for d in range(1, tp):
        copies[d - 1].wait_recv()
        stat = stat + stat_recv[d - 1]
    average = stat[:, 0:1] / width
    spread = stat[:, 1:2] / width - average * average
    out[...] = (
        (second - average) * lax.rsqrt(spread + norm_epsilon) * second_gain[...]
    ).astype(BF16)
    for copy in sent:
        copy.wait_send()


def shards(
    tokens,
    state,
    w_recep,
    w_key,
    w_value,
    w_out,
    decay_base,
    decay_down,
    decay_up,
    rate_base,
    rate_down,
    rate_up,
    head_gain,
    first_gain,
    expert_gate,
    expert_up,
    expert_down,
    dense_gate,
    dense_up,
    dense_down,
    branch_gate,
    second_gain,
    routes,
    route_weights,
):
    ep, tp = lax.axis_size("ep"), lax.axis_size("tp")
    rows, width = tokens.shape
    quarter = w_recep.shape[1]
    side = tp
    layers = ep // (side * CORES)
    plane = tp * side
    large = (
        state,
        w_recep,
        w_key,
        w_value,
        w_out,
        decay_down.T,
        decay_up,
        rate_down.T,
        rate_up,
        expert_gate[0].T,
        expert_up[0].T,
        expert_down[0],
        dense_gate,
        dense_up,
        dense_down,
    )
    small = (
        tokens,
        decay_base[None],
        rate_base[None],
        head_gain[None],
        first_gain[None],
        branch_gate,
        second_gain[None],
        routes.T,
        route_weights.T,
    )
    dma = pltpu.SemaphoreType.DMA
    return pl.pallas_call(
        functools.partial(layer_kernel, ep, tp),
        out_shape=jax.ShapeDtypeStruct((rows, quarter), BF16),
        in_specs=[pl.BlockSpec(memory_space=pltpu.VMEM)] * len(small)
        + [pl.BlockSpec(memory_space=pl.ANY)] * len(large),
        out_specs=pl.BlockSpec(memory_space=pltpu.VMEM),
        scratch_shapes=[pltpu.VMEM(a.shape, a.dtype) for a in large]
        + [
            pltpu.VMEM((rows, width), BF16),
            pltpu.VMEM((tp - 1, rows, width), BF16),
            pltpu.VMEM((ep, rows, width + LANES), BF16),
            pltpu.VMEM((layers, CORES, plane, rows, quarter), BF16),
            pltpu.VMEM((layers, plane, rows, quarter), BF16),
            pltpu.VMEM((layers, plane, rows, quarter), BF16),
            pltpu.VMEM((layers, plane - 1, rows, quarter), BF16),
            pltpu.VMEM((layers - 1, rows, quarter), BF16),
            pltpu.VMEM((layers - 1, rows, quarter), BF16),
            pltpu.VMEM((rows, LANES), F32),
            pltpu.VMEM((tp - 1, rows, LANES), F32),
            dma((len(large),)),
            dma((tp - 1, 2)),
            dma((layers - 1, 2)),
            dma((layers, side - 1, 2)),
            dma((layers, side, 2)),
            dma((layers, 2)),
            dma((layers, plane - 1, 2)),
            dma((layers - 1, 2)),
            dma((tp - 1, 2)),
        ],
        compiler_params=pltpu.CompilerParams(collective_id=0, has_side_effects=True),
    )(*small, *large)


def solution(mesh):
    return jax.shard_map(
        shards,
        mesh=mesh,
        in_specs=(
            P("ep", None),
            P("ep", "tp", None, None),
            P(None, "tp"),
            P(None, "tp"),
            P(None, "tp"),
            P("tp", None),
            P("tp"),
            P(),
            P(None, "tp"),
            P("tp"),
            P(),
            P(None, "tp"),
            P("tp"),
            P(),
            P("ep", None, "tp"),
            P("ep", None, "tp"),
            P("ep", "tp", None),
            P("ep", None),
            P("ep", None),
            P("ep", "tp"),
            P(),
            P("tp"),
            P("ep", None),
            P("ep", None),
        ),
        out_specs=P("ep", "tp"),
        check_vma=False,
    )
```
